32 devices in a mesh: ep: 8 (over z, y), tp: 4 (over x, core).
Axes of the slice: x: 2, y: 2, z: 4, core: 2. Of those that a mesh axis runs over, the one named last changes fastest.
Arguments:
- tokens: bfloat16 [128, 1024], P('ep', 'tp'), may hold values from -75 to 75
- gain_mix: float32 [1024], replicated, may hold values from 0.1 to 1.9
- w_query: bfloat16 [1024, 512], P(None, 'tp'), may hold values from -0.1875 to 0.1875
- w_key: bfloat16 [1024, 512], P(None, 'tp'), may hold values from -0.1875 to 0.1875
- w_value: bfloat16 [1024, 512], P(None, 'tp'), may hold values from -0.1875 to 0.1875
- w_outgate: bfloat16 [1024, 512], P(None, 'tp'), may hold values from -0.1875 to 0.1875
- w_input_gate: bfloat16 [1024, 4], P(None, 'tp'), may hold values from -0.1875 to 0.1875
- w_forget_gate: bfloat16 [1024, 4], P(None, 'tp'), may hold values from -0.1875 to 0.1875
- w_mix_out: bfloat16 [512, 1024], P(None, 'tp'), may hold values from -0.25 to 0.25
- cell_state: float32 [128, 4, 128, 128], P('ep', 'tp'), may hold values from -3 to 3
- norm_state: float32 [128, 4, 128], P('ep', 'tp'), may hold values from -3 to 3
- max_state: float32 [128, 4], P('ep', 'tp'), may hold values from -2 to 143
- gain_ffn: float32 [1024], replicated, may hold values from 0.1 to 1.9
- route_ids: int32 [128, 2], P('ep'), may hold values from 0 to 7, all different within a row; in each aligned block of 16 rows (0 to 15, 16 to 31, ...) at most 8 rows name the same one
- route_logits: float32 [128, 2], P('ep'), may hold values from -5 to 5
- expert_gate: bfloat16 [8, 1024, 1408], P('ep', None, 'tp'), may hold values from -0.1875 to 0.1875
- expert_up: bfloat16 [8, 1024, 1408], P('ep', None, 'tp'), may hold values from -0.1875 to 0.1875
- expert_down: bfloat16 [8, 1408, 1024], P('ep', 'tp'), may hold values from -0.15625 to 0.15625
- dense_gate: bfloat16 [1024, 3072], P('tp', 'ep'), may hold values from -0.1875 to 0.1875
- dense_up: bfloat16 [1024, 3072], P('tp', 'ep'), may hold values from -0.1875 to 0.1875
- dense_down: bfloat16 [3072, 1024], P('ep', 'tp'), may hold values from -0.3125 to 0.3125
- dense_mix: bfloat16 [1024], P('tp'), may hold values from -0.1875 to 0.1875
Outputs:
- layer_out: bfloat16 [128, 1024], P('ep', 'tp')
The draws below stay inside these ranges and needn't reach their ends.
Inputs may be any that keep to these rules, and one draw needn't show every extreme that they name: `route_ids`: each row names 2 different experts. Among the 16 tokens of one index of ep no expert is named more than 8 times, and in every draw some expert is named exactly 8 times by the tokens of one index of ep.
All inputs are finite; a program needn't handle non-finite values.
Results may differ from the reference program's by a relative error of at most 0.013.
Values may be sent and summed in bfloat16 or wider, within the bound.
A program may use at most 64 MiB of HBM per device.

```python
import math
import jax
import jax.numpy as jnp
import numpy as np
from jax import lax

D = 1024
HEADS = 4
HEAD = 128
FF_EXP = 1408
DENSE_FF = 3072
SEQ_DEV = 16
TOP = 2
CAP = 8
WIDTH = 512
BATCH = 128
EXPERTS = 8
N_TP = 4


def draw_tokens(key, part):
    key_base, key_group, key_block = jax.random.split(key, 3)
    base = jnp.clip(jax.random.normal(key_base, (BATCH, D), jnp.float32), -5.0, 5.0)
    group_scale = jnp.exp(jax.random.uniform(key_group, (D // 16,), jnp.float32, -1.1, 1.1))
    block_scale = jnp.exp(jax.random.uniform(key_block, (4,), jnp.float32, -1.1, 1.1))
    columns = jnp.arange(D)
    values = base * group_scale[columns // 16][None, :] * block_scale[columns // (D // 4)][None, :]
    return values.astype(jnp.bfloat16)


def draw_max_state(key, part):
    key_base = jax.random.fold_in(key, 0)
    base = jax.random.uniform(key_base, (BATCH, HEADS), jnp.float32, -2.0, 3.0)
    return base


def shard_levels(stream_key, dims, cuts, low, top_value):
    level, own = 1.0, jax.random.fold_in(stream_key, 6)
    for position, parts in cuts:
        heights = jnp.exp(jax.random.uniform(jax.random.fold_in(own, position), (parts,), jnp.float32, low / len(cuts), top_value / len(cuts)))
        level = level * jnp.repeat(heights, dims[position] // parts).reshape([-1 if axis == position else 1 for axis in range(len(dims))])
    return level


def deal_out(stream_key, own, number, rows, amount, top, limit, skew):
    sequence = jax.random.permutation(stream_key, amount)
    heavy_load, ordinary = load_shares(amount, rows * top, limit, skew, True), load_shares(amount, rows * top, limit, skew, False)
    places = jnp.arange(amount)

    def named(tallies, rotation):
        used = int((tallies > 0).sum())
        fixed = max(1, used // 4)
        passed = fixed + (places - fixed + rotation * (used - fixed)) % max(1, amount - fixed)
        return jnp.zeros((amount,), jnp.int32).at[sequence[jnp.where(places < fixed, places, passed)]].set(jnp.asarray(tallies, jnp.int32))

    tallies = jnp.where(number % 4 == 0, named(heavy_load, number // 4), named(ordinary, number - number // 4 - 1))
    mixed = jax.random.permutation(jax.random.fold_in(own, 3), amount)
    giver, sink = mixed[0:amount // 2 * 2:2], mixed[1:amount // 2 * 2:2]
    room = jnp.minimum(tallies[giver] - 1, limit - tallies[sink]) // 2
    room = jnp.where((giver == sequence[0]) | (sink == sequence[0]) | (tallies[sink] == 0), 0, jnp.maximum(room, 0))
    passed = jax.random.randint(jax.random.fold_in(own, 4), (amount // 2,), 0, 1 << 20) % (room + 1)
    tallies = tallies.at[giver].add(-passed).at[sink].add(passed)
    members = jnp.searchsorted(jnp.cumsum(tallies), jnp.arange(rows * top), side="right").astype(jnp.int32)
    table = members.reshape(top, rows).T
    table = table[jax.random.permutation(jax.random.fold_in(own, 1), rows)]
    rotation = jax.random.randint(jax.random.fold_in(own, 2), (rows, 1), 0, top)
    return jnp.take_along_axis(table, (jnp.arange(top)[None, :] + rotation) % top, axis=1)


def load_shares(count, total, most, skew, full):
    weights = [(1 << 20) // math.isqrt(standing ** skew) + 1 for standing in range(1, count + 1)]
    largest = most if full else min(most, max(-(-total // count), total * weights[0] // sum(weights)))
    least = 1 if total - largest >= count - 1 else 0
    counts, spare = [largest] + [least] * (count - 1), total - largest - least * (count - 1)
    while spare > 0:
        free = [i for i in range(1, count) if counts[i] < largest] or [i for i in range(1, count) if counts[i] < most]
        mass, budget = sum([weights[i] for i in free]), spare
        for i in free:
            more = min(most - counts[i], max(1, budget * weights[i] // mass), spare)
            counts[i] = counts[i] + more
            spare = spare - more
    return np.array(counts)


def normal_values(key, dims, scale, bound, shards=(), held_as=jnp.bfloat16):
    factor_of = shard_levels(key, dims, shards, -0.22, 0.18) if shards else 1.0
    drawn = jax.random.normal(key, dims, jnp.float32) * scale * factor_of
    return jnp.minimum(jnp.maximum(drawn, -bound), bound).astype(held_as)


def setup_inputs(seed: int = 0) -> dict:
    key_of = jax.random.split(jax.random.key(seed), 23)
    tokens = draw_tokens(jax.random.fold_in(key_of[22], 71), 0)
    gain_mix = jnp.clip(1.0 + 0.18 * jax.random.normal(key_of[1], (D,), jnp.float32), 0.1, 1.9)
    w_query = normal_values(key_of[2], (D, WIDTH), D ** -0.5, 0.1875, ((1, 4),))
    w_key = normal_values(key_of[3], (D, WIDTH), D ** -0.5, 0.1875, ((1, 4),))
    w_value = normal_values(key_of[4], (D, WIDTH), D ** -0.5, 0.1875, ((1, 4),))
    w_outgate = normal_values(key_of[5], (D, WIDTH), D ** -0.5, 0.1875, ((1, 4),))
    w_input_gate = normal_values(key_of[6], (D, HEADS), D ** -0.5, 0.1875, ((1, 4),))
    w_forget_gate = normal_values(key_of[7], (D, HEADS), D ** -0.5, 0.1875, ((1, 4),))
    w_mix_out = normal_values(key_of[8], (WIDTH, D), WIDTH ** -0.5, 0.25, ((1, 4),))
    cell_state = normal_values(key_of[9], (BATCH, HEADS, HEAD, HEAD), 0.5, 3.0, ((0, 8), (1, 4)), jnp.float32)
    norm_state = normal_values(key_of[10], (BATCH, HEADS, HEAD), 0.5, 3.0, ((0, 8), (1, 4)), jnp.float32)
    max_state = draw_max_state(jax.random.fold_in(key_of[22], 71), 0)
    gain_ffn = jnp.clip(1.0 + 0.18 * jax.random.normal(key_of[12], (D,), jnp.float32), 0.1, 1.9)
    route_ids_keys = jax.random.split(jax.random.fold_in(key_of[13], 1), BATCH // SEQ_DEV)
    route_ids_turns = jax.random.permutation(jax.random.fold_in(key_of[13], 3), BATCH // SEQ_DEV)
    route_ids = jax.vmap(lambda own, number: deal_out(jax.random.fold_in(key_of[13], 2), own, number, SEQ_DEV, EXPERTS, TOP, CAP, 2))(route_ids_keys, route_ids_turns).reshape((BATCH, TOP))
    route_logits = normal_values(key_of[14], (BATCH, TOP), 1.0, 5.0, ((0, 8),), jnp.float32)
    expert_gate = normal_values(key_of[15], (EXPERTS, D, FF_EXP), D ** -0.5, 0.1875, ((0, 8), (2, 4)))
    expert_up = normal_values(key_of[16], (EXPERTS, D, FF_EXP), D ** -0.5, 0.1875, ((0, 8), (2, 4)))
    expert_down = normal_values(key_of[17], (EXPERTS, FF_EXP, D), FF_EXP ** -0.5, 0.15625, ((0, 8), (1, 4)))
    dense_gate = normal_values(key_of[18], (D, DENSE_FF), D ** -0.5, 0.1875, ((0, 4), (1, 8)))
    dense_up = normal_values(key_of[19], (D, DENSE_FF), D ** -0.5, 0.1875, ((0, 4), (1, 8)))
    dense_down = normal_values(key_of[20], (DENSE_FF, D), (DENSE_FF // 8) ** -0.5, 0.3125, ((0, 8), (1, 4)))
    dense_mix = normal_values(key_of[21], (D,), D ** -0.5, 0.1875, ((0, 4),))
    return dict(tokens=tokens, gain_mix=gain_mix, w_query=w_query, w_key=w_key, w_value=w_value, w_outgate=w_outgate, w_input_gate=w_input_gate, w_forget_gate=w_forget_gate, w_mix_out=w_mix_out, cell_state=cell_state, norm_state=norm_state, max_state=max_state, gain_ffn=gain_ffn, route_ids=route_ids, route_logits=route_logits, expert_gate=expert_gate, expert_up=expert_up, expert_down=expert_down, dense_gate=dense_gate, dense_up=dense_up, dense_down=dense_down, dense_mix=dense_mix)


epsilon = 1e-06
highest = lax.Precision.HIGHEST

def rms_norm(rows, gain):
    values = rows.astype(jnp.float32)
    scale = lax.rsqrt(lax.optimization_barrier(jnp.mean(values * values, axis=-1, keepdims=True)) + epsilon)
    return (values * scale * gain).astype(jnp.bfloat16)

def reference(tokens, gain_mix, w_query, w_key, w_value, w_outgate, w_input_gate, w_forget_gate, w_mix_out, cell_state, norm_state, max_state, gain_ffn, route_ids, route_logits, expert_gate, expert_up, expert_down, dense_gate, dense_up, dense_down, dense_mix):
    normed_mix = rms_norm(tokens, gain_mix)

    def project(weight):
        return jnp.dot(normed_mix, weight, preferred_element_type=jnp.float32)
    query_rows = project(w_query).reshape(BATCH, HEADS, HEAD)
    key_rows = project(w_key).reshape(BATCH, HEADS, HEAD) * HEAD ** (-0.5)
    value_rows = project(w_value).reshape(BATCH, HEADS, HEAD)
    out_gate = project(w_outgate)
    input_gate = project(w_input_gate)
    carried = jax.nn.log_sigmoid(project(w_forget_gate)) + max_state
    stabilizer = jnp.maximum(carried, input_gate)
    weight_old = jnp.exp(carried - stabilizer)
    weight_new = jnp.exp(input_gate - stabilizer) * lax.optimization_barrier(jnp.sum(query_rows * key_rows, axis=-1))
    cell_read = jnp.einsum('bhd,bhde->bhe', query_rows, cell_state, precision=highest)
    numerator = weight_old[..., None] * cell_read + weight_new[..., None] * value_rows
    denominator = weight_old * lax.optimization_barrier(jnp.sum(query_rows * norm_state, axis=-1)) + weight_new
    cell_out = numerator / jnp.maximum(jnp.abs(denominator), 1.0)[..., None]
    mixed = (jax.nn.sigmoid(out_gate) * cell_out.reshape(BATCH, WIDTH)).astype(jnp.bfloat16)
    resid = (tokens.astype(jnp.float32) + jnp.dot(mixed, w_mix_out, preferred_element_type=jnp.float32)).astype(jnp.bfloat16)
    normed_ffn = rms_norm(resid, gain_ffn)
    route_weight = jax.nn.sigmoid(route_logits - route_logits[:, ::-1])
    token_rows = jnp.repeat(normed_ffn, TOP, axis=0)
    flat_ids = route_ids.reshape(-1).astype(jnp.int32)

    def apply_expert(assignment):
        token_row, expert_id = assignment
        gate_rows = jnp.dot(token_row, expert_gate[expert_id], preferred_element_type=jnp.float32)
        up_rows = jnp.dot(token_row, expert_up[expert_id], preferred_element_type=jnp.float32)
        hidden = (jax.nn.silu(gate_rows) * up_rows).astype(jnp.bfloat16).reshape(N_TP, FF_EXP // N_TP)
        down_rows = expert_down[expert_id].reshape(N_TP, FF_EXP // N_TP, D).astype(jnp.float32)
        blocks = jnp.einsum('jf,jfd->jd', hidden.astype(jnp.float32), down_rows, precision=highest)
        blocks = lax.optimization_barrier(blocks.astype(jnp.bfloat16))
        return lax.optimization_barrier(jnp.sum(blocks.astype(jnp.float32), axis=0)).astype(jnp.bfloat16)
    expert_result = lax.map(apply_expert, (token_rows, flat_ids)).reshape(BATCH, TOP, D)
    moe = lax.optimization_barrier(jnp.sum(route_weight[..., None] * expert_result.astype(jnp.float32), axis=1))
    dense_g = jnp.dot(normed_ffn, dense_gate, preferred_element_type=jnp.float32)
    dense_u = jnp.dot(normed_ffn, dense_up, preferred_element_type=jnp.float32)
    dense_hidden = (jax.nn.silu(dense_g) * dense_u).astype(jnp.bfloat16)
    dense_out = jnp.dot(dense_hidden, dense_down, preferred_element_type=jnp.float32)
    mix_gate = jax.nn.sigmoid(jnp.dot(normed_ffn, dense_mix, preferred_element_type=jnp.float32))
    total = resid.astype(jnp.float32) + moe + mix_gate[:, None] * dense_out
    return total.astype(jnp.bfloat16)
```

```python
import functools

import jax
import jax.numpy as jnp
from jax import lax
from jax.experimental import pallas as pl
from jax.experimental.pallas import tpu as pltpu
from jax.sharding import PartitionSpec as P

F32 = jnp.float32
BF16 = jnp.bfloat16
MESH = pl.DeviceIdType.MESH
EPS = 1e-06


def dot(a, b):
    return jnp.dot(a, b, preferred_element_type=F32)


def kernel(
    n_ep,
    n_tp,
    tokens,
    gain_mix,
    w_ig,
    w_fg,
    norm_state,
    max_state,
    gain_ffn,
    ids,
    logits,
    dense_mix,
    w_q,
    w_k,
    w_v,
    w_o,
    w_mix,
    cell,
    e_gate,
    e_up,
    e_down,
    d_gate,
    d_up,
    d_down,
    out,
    wp,
    wm,
    cs,
    eg,
    eu,
    ed,
    dg,
    du,
    dd,
    tok_all,
    mix_all,
    mix_own,
    dm_own,
    dm_all,
    rw_own,
    rw_all,
    res_own,
    res_all,
    xs,
    read,
    c_out,
    c_in,
    local_sem,
    send_sem,
    recv_sem,
    bulk_send,
    bulk_recv,
):
    i = lax.axis_index("ep")
    j = lax.axis_index("tp")
    n_all = n_ep * n_tp
    me = i * n_tp + j
    seq, quarter = tokens.shape
    head = cs.shape[-1]

    local = []

    def fetch(src, dst):
        copy = pltpu.make_async_copy(src, dst, local_sem.at[len(local)])
        copy.start()
        local.append(copy)
        return copy

    barrier = pltpu.get_barrier_semaphore()

    def greet(step, carry):
        peer = lax.rem(me + step, n_all)
        pl.semaphore_signal(
            barrier,
            inc=1,
            device_id=(peer // n_tp, lax.rem(peer, n_tp)),
            device_id_type=MESH,
        )
        return carry

    lax.fori_loop(1, n_all, greet, 0)

    got_proj = [
        fetch(w, wp.at[:, pl.ds(k * head, head)]) for k, w in enumerate((w_q, w_k, w_v, w_o))
    ]
    got_cell = fetch(cell, cs)
    got_mix = fetch(w_mix, wm)
    got_eg = fetch(e_gate.at[0], eg)
    got_eu = fetch(e_up.at[0], eu)
    got_ed = fetch(e_down.at[0], ed)
    got_dg = fetch(d_gate, dg.at[j])
    got_du = fetch(d_up, du.at[j])
    got_dd = fetch(d_down, dd)

    lane = lax.broadcasted_iota(jnp.int32, rw_own.shape, 1)
    l0, l1 = logits[:, 0:1], logits[:, 1:2]
    rw_own[...] = jnp.where(lane == ids[:, 0:1], jax.nn.sigmoid(l0 - l1), 0.0) + jnp.where(
        lane == ids[:, 1:2], jax.nn.sigmoid(l1 - l0), 0.0
    )
    rw_all[i] = rw_own[...]
    dm_own[...] = jnp.broadcast_to(dense_mix[...].astype(F32), dm_own.shape)
    dm_all[j] = dm_own[...]
    tok_all[j] = tokens[...]

    pl.semaphore_wait(barrier, n_all - 1)

    def to_tp(src, dst, phase):
        for step in range(1, n_tp):
            pltpu.make_async_remote_copy(
                src_ref=src,
                dst_ref=dst.at[j],
                send_sem=send_sem.at[phase],
                recv_sem=recv_sem.at[phase],
                device_id=(i, lax.rem(j + step, n_tp)),
                device_id_type=MESH,
            ).start()

    def wait_bytes(buf, count, sem):
        view = buf.at[pl.ds(0, count)]
        pltpu.make_async_copy(view, view, sem).wait()

    to_tp(tokens, tok_all, 0)

    near = j + 1 - 2 * lax.rem(j, 2)
    far = lax.rem(j + 2, n_tp)

    def bulk(src, buf, slot, peer, k):
        return pltpu.make_async_remote_copy(
            src_ref=src,
            dst_ref=buf.at[slot],
            send_sem=bulk_send.at[k],
            recv_sem=bulk_recv.at[k],
            device_id=(i, peer),
            device_id_type=MESH,
        )

    gate_far = bulk(d_gate, dg, j, far, 0)
    gate_near = bulk(d_gate, dg, j, near, 1)
    gate_on = bulk(dg.at[far], dg, far, near, 2)
    up_far = bulk(d_up, du, j, far, 3)
    up_near = bulk(d_up, du, j, near, 4)
    up_on = bulk(du.at[far], du, far, near, 5)
    gate_far.start()
    gate_near.start()

    def send_rw(step, carry):
        pltpu.make_async_remote_copy(
            src_ref=rw_own,
            dst_ref=rw_all.at[i],
            send_sem=send_sem.at[1],
            recv_sem=recv_sem.at[1],
            device_id=(lax.rem(i + step, n_ep), j),
            device_id_type=MESH,
        ).start()
        return carry

    lax.fori_loop(1, n_ep, send_rw, 0)
    to_tp(dm_own, dm_all, 2)

    wait_bytes(tok_all, n_tp - 1, recv_sem.at[0])
    full = jnp.concatenate([tok_all[k] for k in range(n_tp)], axis=1).astype(F32)
    scale = lax.rsqrt(jnp.mean(full * full, axis=-1, keepdims=True) + EPS)
    normed = (full * scale * gain_mix[...]).astype(BF16)
    normed_f = normed.astype(F32)
    ig = jnp.sum(normed_f * w_ig[...].astype(F32), axis=-1, keepdims=True)
    fg = jnp.sum(normed_f * w_fg[...].astype(F32), axis=-1, keepdims=True)
    for copy in got_proj:
        copy.wait()
    proj = dot(normed, wp[...])
    query = proj[:, :head]
    key = proj[:, head : 2 * head] * head ** (-0.5)
    value = proj[:, 2 * head : 3 * head]
    out_gate = proj[:, 3 * head :]
    carried = jnp.minimum(fg, 0.0) - jnp.log1p(jnp.exp(-jnp.abs(fg))) + max_state[...]
    stab = jnp.maximum(carried, ig)
    w_old = jnp.exp(carried - stab)
    w_new = jnp.exp(ig - stab) * jnp.sum(query * key, axis=-1, keepdims=True)
    got_cell.wait()
    query_t = query.T
    for b in range(seq):
        read[b : b + 1, :] = jnp.sum(query_t[:, b : b + 1] * cs[b], axis=0, keepdims=True)
    numer = w_old * read[...] + w_new * value
    denom = w_old * jnp.sum(query * norm_state[...], axis=-1, keepdims=True) + w_new
    cell_out = numer / jnp.maximum(jnp.abs(denom), 1.0)
    mixed = (jax.nn.sigmoid(out_gate) * cell_out).astype(BF16)
    mix_own[...] = mixed
    mix_all[j] = mixed
    to_tp(mix_own, mix_all, 3)
    got_mix.wait()
    wait_bytes(mix_all, n_tp - 1, recv_sem.at[3])
    heads = jnp.concatenate([mix_all[k] for k in range(n_tp)], axis=1)
    resid = (tokens[...].astype(F32) + dot(heads, wm[...])).astype(BF16)
    res_own[...] = resid
    res_all[me] = resid

    def send_res(step, carry):
        peer = lax.rem(me + step, n_all)
        pltpu.make_async_remote_copy(
            src_ref=res_own,
            dst_ref=res_all.at[me],
            send_sem=send_sem.at[4],
            recv_sem=recv_sem.at[4],
            device_id=(peer // n_tp, lax.rem(peer, n_tp)),
            device_id_type=MESH,
        ).start()
        return carry

    lax.fori_loop(1, n_all, send_res, 0)
    up_far.start()
    up_near.start()
    gate_far.wait_recv()
    gate_on.start()

    wait_bytes(rw_all, n_ep - 1, recv_sem.at[1])
    rw = rw_all[...].reshape(n_ep * seq, -1)
    lanes = lax.broadcasted_iota(jnp.int32, rw.shape, 1)
    weight = jnp.sum(jnp.where(lanes == i, rw, 0.0), axis=-1, keepdims=True)
    wait_bytes(dm_all, n_tp - 1, recv_sem.at[2])

    wait_bytes(res_all, n_all - 1, recv_sem.at[4])
    rows = res_all[...].reshape(n_ep, n_tp, seq, quarter)
    parts = [rows[:, k].reshape(n_ep * seq, quarter).astype(F32) for k in range(n_tp)]
    square = sum(jnp.sum(p * p, axis=-1, keepdims=True) for p in parts)
    scale = lax.rsqrt(square / (n_tp * quarter) + EPS)
    logit = jnp.zeros_like(scale)
    for k in range(n_tp):
        cols = slice(k * quarter, (k + 1) * quarter)
        part = (parts[k] * scale * gain_ffn[:, cols]).astype(BF16)
        xs[:, cols] = part
        logit += jnp.sum(part.astype(F32) * dm_all[k][0:1, :], axis=-1, keepdims=True)
    mix_gate = jax.nn.sigmoid(logit)

    got_eg.wait()
    got_eu.wait()
    g = dot(xs[...], eg[...])
    u = dot(xs[...], eu[...])
    hidden = (g * jax.nn.sigmoid(g) * u).astype(BF16)
    up_far.wait_recv()
    up_on.start()
    got_ed.wait()
    part = dot(hidden, ed[...]) * weight

    got_dg.wait()
    gate_near.wait_recv()
    gate_on.wait_recv()
    g = dot(xs[...], dg[...].reshape(n_tp * quarter, -1))
    got_du.wait()
    up_near.wait_recv()
    up_on.wait_recv()
    u = dot(xs[...], du[...].reshape(n_tp * quarter, -1))
    hidden = (g * jax.nn.sigmoid(g) * u).astype(BF16)
    got_dd.wait()
    dense = dot(hidden, dd[...]) * mix_gate
    for k in range(n_tp):
        total = part[:, k * quarter : (k + 1) * quarter] + jnp.where(j == k, dense, 0.0)
        c_out[k] = total.astype(BF16).reshape(n_ep, seq, quarter)
    c_in[me] = c_out[j, i]

    def send_back(step, carry):
        peer = lax.rem(me + step, n_all)
        pi, pj = peer // n_tp, lax.rem(peer, n_tp)
        pltpu.make_async_remote_copy(
            src_ref=c_out.at[pj, pi],
            dst_ref=c_in.at[me],
            send_sem=send_sem.at[5],
            recv_sem=recv_sem.at[5],
            device_id=(pi, pj),
            device_id_type=MESH,
        ).start()
        return carry

    lax.fori_loop(1, n_all, send_back, 0)

    wait_bytes(tok_all, n_tp - 1, send_sem.at[0])
    wait_bytes(rw_all, n_ep - 1, send_sem.at[1])
    wait_bytes(dm_all, n_tp - 1, send_sem.at[2])
    wait_bytes(mix_all, n_tp - 1, send_sem.at[3])
    wait_bytes(res_all, n_all - 1, send_sem.at[4])
    for copy in (gate_far, gate_near, gate_on, up_far, up_near, up_on):
        copy.wait_send()

    wait_bytes(c_in, n_all - 1, recv_sem.at[5])

    def add(k, total):
        return total + c_in[k].astype(F32)

    total = lax.fori_loop(0, n_all, add, res_own[...].astype(F32), unroll=min(8, n_all))
    out[...] = total.astype(BF16)
    wait_bytes(c_in, n_all - 1, send_sem.at[5])


def local(
    n_ep,
    n_tp,
    tokens,
    gain_mix,
    w_query,
    w_key,
    w_value,
    w_outgate,
    w_input_gate,
    w_forget_gate,
    w_mix_out,
    cell_state,
    norm_state,
    max_state,
    gain_ffn,
    route_ids,
    route_logits,
    expert_gate,
    expert_up,
    expert_down,
    dense_gate,
    dense_up,
    dense_down,
    dense_mix,
):
    seq, quarter = tokens.shape
    features, head = w_query.shape
    n_all = n_ep * n_tp
    lanes = -(-n_ep // 128) * 128
    ff = expert_gate.shape[2]
    dff = dense_gate.shape[1]
    vmem = pl.BlockSpec(memory_space=pltpu.VMEM)
    any_space = pl.BlockSpec(memory_space=pl.ANY)
    small = (
        tokens,
        gain_mix.reshape(1, -1),
        w_input_gate.reshape(1, -1),
        w_forget_gate.reshape(1, -1),
        norm_state.reshape(seq, head),
        max_state,
        gain_ffn.reshape(1, -1),
        route_ids,
        route_logits,
        dense_mix.reshape(1, -1),
    )
    large = (
        w_query,
        w_key,
        w_value,
        w_outgate,
        w_mix_out,
        cell_state.reshape(seq, head, head),
        expert_gate,
        expert_up,
        expert_down,
        dense_gate,
        dense_up,
        dense_down,
    )
    return pl.pallas_call(
        functools.partial(kernel, n_ep, n_tp),
        out_shape=jax.ShapeDtypeStruct((seq, quarter), BF16),
        in_specs=[vmem] * len(small) + [any_space] * len(large),
        out_specs=vmem,
        scratch_shapes=[
            pltpu.VMEM((features, 4 * head), BF16),
            pltpu.VMEM(w_mix_out.shape, BF16),
            pltpu.VMEM((seq, head, head), F32),
            pltpu.VMEM((features, ff), BF16),
            pltpu.VMEM((features, ff), BF16),
            pltpu.VMEM((ff, features), BF16),
            pltpu.VMEM((n_tp, quarter, dff), BF16),
            pltpu.VMEM((n_tp, quarter, dff), BF16),
            pltpu.VMEM(dense_down.shape, BF16),
            pltpu.VMEM((n_tp, seq, quarter), BF16),
            pltpu.VMEM((n_tp, seq, head), BF16),
            pltpu.VMEM((seq, head), BF16),
            pltpu.VMEM((8, quarter), F32),
            pltpu.VMEM((n_tp, 8, quarter), F32),
            pltpu.VMEM((seq, lanes), F32),
            pltpu.VMEM((n_ep, seq, lanes), F32),
            pltpu.VMEM((seq, quarter), BF16),
            pltpu.VMEM((n_all, seq, quarter), BF16),
            pltpu.VMEM((n_ep * seq, features), BF16),
            pltpu.VMEM((seq, head), F32),
            pltpu.VMEM((n_tp, n_ep, seq, quarter), BF16),
            pltpu.VMEM((n_all, seq, quarter), BF16),
            pltpu.SemaphoreType.DMA((12,)),
            pltpu.SemaphoreType.DMA((6,)),
            pltpu.SemaphoreType.DMA((6,)),
            pltpu.SemaphoreType.DMA((6,)),
            pltpu.SemaphoreType.DMA((6,)),
        ],
        compiler_params=pltpu.CompilerParams(
            collective_id=0, has_side_effects=True, vmem_limit_bytes=60 * 1024 * 1024
        ),
    )(*small, *large)


def solution(mesh):
    return jax.shard_map(
        functools.partial(local, mesh.shape["ep"], mesh.shape["tp"]),
        mesh=mesh,
        in_specs=(
            P("ep", "tp"),
            P(),
            P(None, "tp"),
            P(None, "tp"),
            P(None, "tp"),
            P(None, "tp"),
            P(None, "tp"),
            P(None, "tp"),
            P(None, "tp"),
            P("ep", "tp", None, None),
            P("ep", "tp", None),
            P("ep", "tp"),
            P(),
            P("ep", None),
            P("ep", None),
            P("ep", None, "tp"),
            P("ep", None, "tp"),
            P("ep", "tp", None),
            P("tp", "ep"),
            P("tp", "ep"),
            P("ep", "tp"),
            P("tp"),
        ),
        out_specs=P("ep", "tp"),
        check_vma=False,
    )
```

```python
import functools

import jax
import jax.numpy as jnp
from jax import lax
from jax.experimental import pallas as pl
from jax.experimental.pallas import tpu as pltpu
from jax.sharding import PartitionSpec as P

F32 = jnp.float32
BF16 = jnp.bfloat16
MESH = pl.DeviceIdType.MESH
EPS = 1e-06


def dot(a, b):
    return jnp.dot(a, b, preferred_element_type=F32)


def dot_t(a, b):
    return lax.dot_general(a, b, (((1,), (1,)), ((), ())), preferred_element_type=F32)


def column(row):
    n = row.shape[1]
    square = (n, n)
    eye = lax.broadcasted_iota(jnp.int32, square, 0) == lax.broadcasted_iota(jnp.int32, square, 1)
    return jnp.sum(jnp.where(eye, jnp.broadcast_to(row, square), 0.0), axis=1, keepdims=True)


def kernel(
    n_ep,
    n_tp,
    tokens,
    gain_mix,
    w_ig,
    w_fg,
    norm_state,
    max_state,
    gain_ffn,
    ids,
    logits,
    dense_mix,
    w_q,
    w_k,
    w_v,
    w_o,
    w_mix,
    cell,
    e_gate,
    e_up,
    e_down,
    d_gate,
    d_up,
    d_down,
    out,
    wp,
    wm,
    cs,
    eg,
    eu,
    ed,
    dg,
    du,
    dd,
    tok_all,
    mix_all,
    mix_own,
    dm_own,
    dm_all,
    rw_own,
    rw_all,
    res_own,
    res_all,
    xs,
    read,
    c_out,
    c_in,
    local_sem,
    send_sem,
    recv_sem,
    bulk_send,
    bulk_recv,
):
    i = lax.axis_index("ep")
    j = lax.axis_index("tp")
    n_all = n_ep * n_tp
    me = i * n_tp + j
    seq, quarter = tokens.shape
    head = cs.shape[-1]

    local = []

    def fetch(src, dst):
        copy = pltpu.make_async_copy(src, dst, local_sem.at[len(local)])
        copy.start()
        local.append(copy)
        return copy

    barrier = pltpu.get_barrier_semaphore()

    def greet(step, carry):
        peer = lax.rem(me + step, n_all)
        pl.semaphore_signal(
            barrier,
            inc=1,
            device_id=(peer // n_tp, lax.rem(peer, n_tp)),
            device_id_type=MESH,
        )
        return carry

    lax.fori_loop(1, n_all, greet, 0)

    got_proj = [
        fetch(w, wp.at[:, pl.ds(k * head, head)]) for k, w in enumerate((w_q, w_k, w_v, w_o))
    ]
    got_cell = fetch(cell, cs)
    got_mix = fetch(w_mix, wm)
    got_eg = fetch(e_gate.at[0], eg)
    got_eu = fetch(e_up.at[0], eu)
    got_ed = fetch(e_down.at[0], ed)
    got_dg = fetch(d_gate, dg.at[j])
    got_du = fetch(d_up, du.at[j])
    got_dd = fetch(d_down, dd)

    lane = lax.broadcasted_iota(jnp.int32, rw_own.shape, 1)
    l0, l1 = column(logits[0:1, :]), column(logits[1:2, :])
    id0, id1 = (column(ids[k : k + 1, :].astype(F32)).astype(jnp.int32) for k in range(2))
    rw_own[...] = jnp.where(lane == id0, jax.nn.sigmoid(l0 - l1), 0.0) + jnp.where(
        lane == id1, jax.nn.sigmoid(l1 - l0), 0.0
    )
    rw_all[i] = rw_own[...]
    mix_row = dense_mix[...].astype(F32)
    mix_row = jnp.concatenate([mix_row[k : k + 1] for k in range(mix_row.shape[0])], axis=1)
    dm_own[...] = jnp.broadcast_to(mix_row, dm_own.shape)
    dm_all[j] = dm_own[...]
    tok_all[j] = tokens[...]

    pl.semaphore_wait(barrier, n_all - 1)

    def to_tp(src, dst, phase):
        for step in range(1, n_tp):
            pltpu.make_async_remote_copy(
                src_ref=src,
                dst_ref=dst.at[j],
                send_sem=send_sem.at[phase],
                recv_sem=recv_sem.at[phase],
                device_id=(i, lax.rem(j + step, n_tp)),
                device_id_type=MESH,
            ).start()

    def wait_bytes(buf, count, sem):
        view = buf.at[pl.ds(0, count)]
        pltpu.make_async_copy(view, view, sem).wait()

    to_tp(tokens, tok_all, 0)

    near = j + 1 - 2 * lax.rem(j, 2)
    far = lax.rem(j + 2, n_tp)

    def bulk(src, buf, slot, peer, k):
        return pltpu.make_async_remote_copy(
            src_ref=src,
            dst_ref=buf.at[slot],
            send_sem=bulk_send.at[k],
            recv_sem=bulk_recv.at[k],
            device_id=(i, peer),
            device_id_type=MESH,
        )

    gate_far = bulk(d_gate, dg, j, far, 0)
    gate_near = bulk(d_gate, dg, j, near, 1)
    gate_on = bulk(dg.at[far], dg, far, near, 2)
    up_far = bulk(d_up, du, j, far, 3)
    up_near = bulk(d_up, du, j, near, 4)
    up_on = bulk(du.at[far], du, far, near, 5)
    gate_far.start()
    gate_near.start()

    def send_rw(step, carry):
        pltpu.make_async_remote_copy(
            src_ref=rw_own,
            dst_ref=rw_all.at[i],
            send_sem=send_sem.at[1],
            recv_sem=recv_sem.at[1],
            device_id=(lax.rem(i + step, n_ep), j),
            device_id_type=MESH,
        ).start()
        return carry

    lax.fori_loop(1, n_ep, send_rw, 0)
    to_tp(dm_own, dm_all, 2)

    wait_bytes(tok_all, n_tp - 1, recv_sem.at[0])
    full = jnp.concatenate([tok_all[k] for k in range(n_tp)], axis=1).astype(F32)
    scale = lax.rsqrt(jnp.mean(full * full, axis=-1, keepdims=True) + EPS)
    normed = (full * scale * gain_mix[...]).astype(BF16)
    normed_f = normed.astype(F32)
    ig = jnp.sum(normed_f * w_ig[...].astype(F32), axis=-1, keepdims=True)
    fg = jnp.sum(normed_f * w_fg[...].astype(F32), axis=-1, keepdims=True)
    for copy in got_proj:
        copy.wait()
    proj = dot(normed, wp[...])
    query = proj[:, :head]
    key = proj[:, head : 2 * head] * head ** (-0.5)
    value = proj[:, 2 * head : 3 * head]
    out_gate = proj[:, 3 * head :]
    carried = jnp.minimum(fg, 0.0) - jnp.log1p(jnp.exp(-jnp.abs(fg))) + column(max_state[...])
    stab = jnp.maximum(carried, ig)
    w_old = jnp.exp(carried - stab)
    w_new = jnp.exp(ig - stab) * jnp.sum(query * key, axis=-1, keepdims=True)
    got_cell.wait()
    query_t = query.T
    for b in range(seq):
        read[b : b + 1, :] = jnp.sum(query_t[:, b : b + 1] * cs[b], axis=0, keepdims=True)
    numer = w_old * read[...] + w_new * value
    denom = w_old * jnp.sum(query * norm_state[...], axis=-1, keepdims=True) + w_new
    cell_out = numer / jnp.maximum(jnp.abs(denom), 1.0)
    mixed = (jax.nn.sigmoid(out_gate) * cell_out).astype(BF16)
    mix_own[...] = mixed
    mix_all[j] = mixed
    to_tp(mix_own, mix_all, 3)
    got_mix.wait()
    wait_bytes(mix_all, n_tp - 1, recv_sem.at[3])
    heads = jnp.concatenate([mix_all[k] for k in range(n_tp)], axis=1)
    resid = (tokens[...].astype(F32) + dot(heads, wm[...])).astype(BF16)
    res_own[...] = resid
    res_all[me] = resid

    def send_res(step, carry):
        peer = lax.rem(me + step, n_all)
        pltpu.make_async_remote_copy(
            src_ref=res_own,
            dst_ref=res_all.at[me],
            send_sem=send_sem.at[4],
            recv_sem=recv_sem.at[4],
            device_id=(peer // n_tp, lax.rem(peer, n_tp)),
            device_id_type=MESH,
        ).start()
        return carry

    lax.fori_loop(1, n_all, send_res, 0)
    up_far.start()
    up_near.start()
    gate_far.wait_recv()
    gate_on.start()

    wait_bytes(rw_all, n_ep - 1, recv_sem.at[1])
    rw = rw_all[...].reshape(n_ep * seq, -1)
    lanes = lax.broadcasted_iota(jnp.int32, rw.shape, 1)
    weight = jnp.sum(jnp.where(lanes == i, rw, 0.0), axis=-1, keepdims=True)
    wait_bytes(dm_all, n_tp - 1, recv_sem.at[2])

    wait_bytes(res_all, n_all - 1, recv_sem.at[4])
    rows = res_all[...].reshape(n_ep, n_tp, seq, quarter)
    parts = [rows[:, k].reshape(n_ep * seq, quarter).astype(F32) for k in range(n_tp)]
    square = sum(jnp.sum(p * p, axis=-1, keepdims=True) for p in parts)
    scale = lax.rsqrt(square / (n_tp * quarter) + EPS)
    logit = jnp.zeros_like(scale)
    for k in range(n_tp):
        cols = slice(k * quarter, (k + 1) * quarter)
        part = (parts[k] * scale * gain_ffn[:, cols]).astype(BF16)
        xs[:, cols] = part
        logit += jnp.sum(part.astype(F32) * dm_all[k][0:1, :], axis=-1, keepdims=True)
    mix_gate = jax.nn.sigmoid(logit)

    got_eg.wait()
    got_eu.wait()
    g = dot_t(xs[...], eg[...])
    u = dot_t(xs[...], eu[...])
    hidden = (g * jax.nn.sigmoid(g) * u).astype(BF16)
    up_far.wait_recv()
    up_on.start()
    got_ed.wait()
    part = dot(hidden, ed[...]) * weight

    got_dg.wait()
    gate_near.wait_recv()
    gate_on.wait_recv()
    g = dot(xs[...], dg[...].reshape(n_tp * quarter, -1))
    got_du.wait()
    up_near.wait_recv()
    up_on.wait_recv()
    u = dot(xs[...], du[...].reshape(n_tp * quarter, -1))
    hidden = (g * jax.nn.sigmoid(g) * u).astype(BF16)
    got_dd.wait()
    dense = dot(hidden, dd[...]) * mix_gate
    for k in range(n_tp):
        total = part[:, k * quarter : (k + 1) * quarter] + jnp.where(j == k, dense, 0.0)
        c_out[k] = total.astype(BF16).reshape(n_ep, seq, quarter)
    c_in[me] = c_out[j, i]

    def send_back(step, carry):
        peer = lax.rem(me + step, n_all)
        pi, pj = peer // n_tp, lax.rem(peer, n_tp)
        pltpu.make_async_remote_copy(
            src_ref=c_out.at[pj, pi],
            dst_ref=c_in.at[me],
            send_sem=send_sem.at[5],
            recv_sem=recv_sem.at[5],
            device_id=(pi, pj),
            device_id_type=MESH,
        ).start()
        return carry

    lax.fori_loop(1, n_all, send_back, 0)

    wait_bytes(tok_all, n_tp - 1, send_sem.at[0])
    wait_bytes(rw_all, n_ep - 1, send_sem.at[1])
    wait_bytes(dm_all, n_tp - 1, send_sem.at[2])
    wait_bytes(mix_all, n_tp - 1, send_sem.at[3])
    wait_bytes(res_all, n_all - 1, send_sem.at[4])
    for copy in (gate_far, gate_near, gate_on, up_far, up_near, up_on):
        copy.wait_send()

    wait_bytes(c_in, n_all - 1, recv_sem.at[5])

    def add(k, total):
        return total + c_in[k].astype(F32)

    total = lax.fori_loop(0, n_all, add, res_own[...].astype(F32), unroll=min(8, n_all))
    out[...] = total.astype(BF16)
    wait_bytes(c_in, n_all - 1, send_sem.at[5])


def local(
    n_ep,
    n_tp,
    tokens,
    gain_mix,
    w_query,
    w_key,
    w_value,
    w_outgate,
    w_input_gate,
    w_forget_gate,
    w_mix_out,
    cell_state,
    norm_state,
    max_state,
    gain_ffn,
    route_ids,
    route_logits,
    expert_gate,
    expert_up,
    expert_down,
    dense_gate,
    dense_up,
    dense_down,
    dense_mix,
):
    seq, quarter = tokens.shape
    features, head = w_query.shape
    n_all = n_ep * n_tp
    lanes = -(-n_ep // 128) * 128
    ff = expert_gate.shape[2]
    dff = dense_gate.shape[1]
    vmem = pl.BlockSpec(memory_space=pltpu.VMEM)
    any_space = pl.BlockSpec(memory_space=pl.ANY)
    small = (
        tokens,
        gain_mix.reshape(1, -1),
        w_input_gate.reshape(1, -1),
        w_forget_gate.reshape(1, -1),
        norm_state.reshape(seq, head),
        max_state.T,
        gain_ffn.reshape(1, -1),
        route_ids.T,
        route_logits.T,
        dense_mix.reshape(-1, 128),
    )
    large = (
        w_query,
        w_key,
        w_value,
        w_outgate,
        w_mix_out,
        cell_state.reshape(seq, head, head),
        jnp.swapaxes(expert_gate, 1, 2),
        jnp.swapaxes(expert_up, 1, 2),
        expert_down,
        dense_gate,
        dense_up,
        dense_down,
    )
    return pl.pallas_call(
        functools.partial(kernel, n_ep, n_tp),
        out_shape=jax.ShapeDtypeStruct((seq, quarter), BF16),
        in_specs=[vmem] * len(small) + [any_space] * len(large),
        out_specs=vmem,
        scratch_shapes=[
            pltpu.VMEM((features, 4 * head), BF16),
            pltpu.VMEM(w_mix_out.shape, BF16),
            pltpu.VMEM((seq, head, head), F32),
            pltpu.VMEM((ff, features), BF16),
            pltpu.VMEM((ff, features), BF16),
            pltpu.VMEM((ff, features), BF16),
            pltpu.VMEM((n_tp, quarter, dff), BF16),
            pltpu.VMEM((n_tp, quarter, dff), BF16),
            pltpu.VMEM(dense_down.shape, BF16),
            pltpu.VMEM((n_tp, seq, quarter), BF16),
            pltpu.VMEM((n_tp, seq, head), BF16),
            pltpu.VMEM((seq, head), BF16),
            pltpu.VMEM((8, quarter), F32),
            pltpu.VMEM((n_tp, 8, quarter), F32),
            pltpu.VMEM((seq, lanes), F32),
            pltpu.VMEM((n_ep, seq, lanes), F32),
            pltpu.VMEM((seq, quarter), BF16),
            pltpu.VMEM((n_all, seq, quarter), BF16),
            pltpu.VMEM((n_ep * seq, features), BF16),
            pltpu.VMEM((seq, head), F32),
            pltpu.VMEM((n_tp, n_ep, seq, quarter), BF16),
            pltpu.VMEM((n_all, seq, quarter), BF16),
            pltpu.SemaphoreType.DMA((12,)),
            pltpu.SemaphoreType.DMA((6,)),
            pltpu.SemaphoreType.DMA((6,)),
            pltpu.SemaphoreType.DMA((6,)),
            pltpu.SemaphoreType.DMA((6,)),
        ],
        compiler_params=pltpu.CompilerParams(
            collective_id=0, has_side_effects=True, vmem_limit_bytes=60 * 1024 * 1024
        ),
    )(*small, *large)


def solution(mesh):
    return jax.shard_map(
        functools.partial(local, mesh.shape["ep"], mesh.shape["tp"]),
        mesh=mesh,
        in_specs=(
            P("ep", "tp"),
            P(),
            P(None, "tp"),
            P(None, "tp"),
            P(None, "tp"),
            P(None, "tp"),
            P(None, "tp"),
            P(None, "tp"),
            P(None, "tp"),
            P("ep", "tp", None, None),
            P("ep", "tp", None),
            P("ep", "tp"),
            P(),
            P("ep", None),
            P("ep", None),
            P("ep", None, "tp"),
            P("ep", None, "tp"),
            P("ep", "tp", None),
            P("tp", "ep"),
            P("tp", "ep"),
            P("ep", "tp"),
            P("tp"),
        ),
        out_specs=P("ep", "tp"),
        check_vma=False,
    )
```

```python
import functools

import jax
import jax.numpy as jnp
from jax import lax
from jax.experimental import pallas as pl
from jax.experimental.pallas import tpu as pltpu
from jax.sharding import PartitionSpec as P

F32 = jnp.float32
BF16 = jnp.bfloat16
MESH = pl.DeviceIdType.MESH
EPS = 1e-06


def dot(a, b):
    return jnp.dot(a, b, preferred_element_type=F32)


def dot_t(a, b):
    return lax.dot_general(a, b, (((1,), (1,)), ((), ())), preferred_element_type=F32)


def column(row):
    n = row.shape[1]
    square = (n, n)
    eye = lax.broadcasted_iota(jnp.int32, square, 0) == lax.broadcasted_iota(jnp.int32, square, 1)
    return jnp.sum(jnp.where(eye, jnp.broadcast_to(row, square), 0.0), axis=1, keepdims=True)


def kernel(
    n_ep,
    n_tp,
    tokens,
    gain_mix,
    w_ig,
    w_fg,
    norm_state,
    max_state,
    gain_ffn,
    ids,
    logits,
    dense_mix,
    w_q,
    w_k,
    w_v,
    w_o,
    w_mix,
    cell,
    e_gate,
    e_up,
    e_down,
    d_gate,
    d_up,
    d_down,
    out,
    wp,
    wm,
    cs,
    eg,
    eu,
    ed,
    dg,
    du,
    dd,
    tok_all,
    mix_all,
    mix_own,
    dm_own,
    dm_all,
    rw_own,
    rw_all,
    res_own,
    res_all,
    xs,
    read,
    give,
    take,
    c_out,
    c_in,
    local_sem,
    send_sem,
    recv_sem,
    bulk_send,
    bulk_recv,
    word_sem,
):
    i = lax.axis_index("ep")
    j = lax.axis_index("tp")
    seq, quarter = tokens.shape
    head = cs.shape[-1]

    local = []

    def fetch(src, dst):
        copy = pltpu.make_async_copy(src, dst, local_sem.at[len(local)])
        copy.start()
        local.append(copy)
        return copy

    barrier = pltpu.get_barrier_semaphore()

    flips = [i + b - 2 * b * lax.rem(i // b, 2) for b in (1 << k for k in range(n_ep.bit_length() - 1))]
    hello = [(i, lax.rem(j + step, n_tp)) for step in range(1, n_tp)] + [(f, j) for f in flips]
    for peer in hello:
        pl.semaphore_signal(barrier, inc=1, device_id=peer, device_id_type=MESH)

    def tell(k):
        pl.semaphore_signal(word_sem.at[k], inc=1, device_id=(flips[k], j), device_id_type=MESH)

    def hear(k):
        pl.semaphore_wait(word_sem.at[k], 1)

    got_proj = [
        fetch(w, wp.at[:, pl.ds(k * head, head)]) for k, w in enumerate((w_q, w_k, w_v, w_o))
    ]
    got_cell = fetch(cell, cs)
    got_mix = fetch(w_mix, wm)
    got_eg = fetch(e_gate.at[0], eg)
    got_eu = fetch(e_up.at[0], eu)
    got_ed = fetch(e_down.at[0], ed)
    got_dg = fetch(d_gate, dg.at[j])
    got_du = fetch(d_up, du.at[j])
    got_dd = fetch(d_down, dd)

    l0, l1 = logits[0:1, :], logits[1:2, :]
    s0, s1 = jax.nn.sigmoid(l0 - l1), jax.nn.sigmoid(l1 - l0)

    def put_rw(e, carry):
        rw_own[e, :, 0:seq] = jnp.where(ids[0:1, :] == e, s0, 0.0) + jnp.where(
            ids[1:2, :] == e, s1, 0.0
        )
        return carry

    rw_own[...] = jnp.zeros_like(rw_own)
    lax.fori_loop(0, n_ep, put_rw, 0, unroll=8)
    rw_all[i] = rw_own[i]
    mix_row = dense_mix[...].astype(F32)
    mix_row = jnp.concatenate([mix_row[k : k + 1] for k in range(mix_row.shape[0])], axis=1)
    dm_own[...] = jnp.broadcast_to(mix_row, dm_own.shape)
    dm_all[j] = dm_own[...]
    tok_all[j] = tokens[...]

    pl.semaphore_wait(barrier, len(hello))
    tell(0)

    def to_tp(src, dst, phase):
        for step in range(1, n_tp):
            pltpu.make_async_remote_copy(
                src_ref=src,
                dst_ref=dst.at[j],
                send_sem=send_sem.at[phase],
                recv_sem=recv_sem.at[phase],
                device_id=(i, lax.rem(j + step, n_tp)),
                device_id_type=MESH,
            ).start()

    def wait_bytes(buf, count, sem):
        view = buf.at[pl.ds(0, count)]
        pltpu.make_async_copy(view, view, sem).wait()

    to_tp(tokens, tok_all, 0)

    near = j + 1 - 2 * lax.rem(j, 2)
    far = lax.rem(j + 2, n_tp)

    def bulk(src, buf, slot, peer, k):
        return pltpu.make_async_remote_copy(
            src_ref=src,
            dst_ref=buf.at[slot],
            send_sem=bulk_send.at[k],
            recv_sem=bulk_recv.at[k],
            device_id=(i, peer),
            device_id_type=MESH,
        )

    gate_far = bulk(d_gate, dg, j, far, 0)
    gate_near = bulk(d_gate, dg, j, near, 1)
    gate_on = bulk(dg.at[far], dg, far, near, 2)
    up_far = bulk(d_up, du, j, far, 3)
    up_near = bulk(d_up, du, j, near, 4)
    up_on = bulk(du.at[far], du, far, near, 5)
    gate_far.start()
    gate_near.start()

    def send_rw(step, carry):
        e = lax.rem(i + step, n_ep)
        pltpu.make_async_remote_copy(
            src_ref=rw_own.at[e],
            dst_ref=rw_all.at[i],
            send_sem=send_sem.at[1],
            recv_sem=recv_sem.at[1],
            device_id=(e, j),
            device_id_type=MESH,
        ).start()
        return carry

    to_tp(dm_own, dm_all, 2)

    wait_bytes(tok_all, n_tp - 1, recv_sem.at[0])
    hear(0)
    tell(1)
    full = jnp.concatenate([tok_all[k] for k in range(n_tp)], axis=1).astype(F32)
    scale = lax.rsqrt(jnp.mean(full * full, axis=-1, keepdims=True) + EPS)
    normed = (full * scale * gain_mix[...]).astype(BF16)
    normed_f = normed.astype(F32)
    ig = jnp.sum(normed_f * w_ig[...].astype(F32), axis=-1, keepdims=True)
    fg = jnp.sum(normed_f * w_fg[...].astype(F32), axis=-1, keepdims=True)
    for copy in got_proj:
        copy.wait()
    proj = dot(normed, wp[...])
    query = proj[:, :head]
    key = proj[:, head : 2 * head] * head ** (-0.5)
    value = proj[:, 2 * head : 3 * head]
    out_gate = proj[:, 3 * head :]
    carried = jnp.minimum(fg, 0.0) - jnp.log1p(jnp.exp(-jnp.abs(fg))) + column(max_state[...])
    stab = jnp.maximum(carried, ig)
    w_old = jnp.exp(carried - stab)
    w_new = jnp.exp(ig - stab) * jnp.sum(query * key, axis=-1, keepdims=True)
    got_cell.wait()
    for k in range(1, len(flips)):
        hear(k)
        if k + 1 < len(flips):
            tell(k + 1)
    query_t = query.T
    for b in range(seq):
        read[b : b + 1, :] = jnp.sum(query_t[:, b : b + 1] * cs[b], axis=0, keepdims=True)
    numer = w_old * read[...] + w_new * value
    denom = w_old * jnp.sum(query * norm_state[...], axis=-1, keepdims=True) + w_new
    cell_out = numer / jnp.maximum(jnp.abs(denom), 1.0)
    mixed = (jax.nn.sigmoid(out_gate) * cell_out).astype(BF16)
    mix_own[...] = mixed
    mix_all[j] = mixed
    to_tp(mix_own, mix_all, 3)
    got_mix.wait()
    wait_bytes(mix_all, n_tp - 1, recv_sem.at[3])
    heads = jnp.concatenate([mix_all[k] for k in range(n_tp)], axis=1)
    resid = (tokens[...].astype(F32) + dot(heads, wm[...])).astype(BF16)
    res_own[...] = resid
    core = lax.rem(j, 2)
    half = n_tp // 2
    n_half = n_ep * half
    mine = i * half + j // 2
    res_all[core, mine] = resid

    def send_res(step, carry):
        peer = lax.rem(mine + step, n_half)
        pltpu.make_async_remote_copy(
            src_ref=res_own,
            dst_ref=res_all.at[core, mine],
            send_sem=send_sem.at[4],
            recv_sem=recv_sem.at[4],
            device_id=(peer // half, 2 * lax.rem(peer, half) + core),
            device_id_type=MESH,
        ).start()
        return carry

    lax.fori_loop(1, n_half, send_res, 0)
    lax.fori_loop(1, n_ep, send_rw, 0)
    up_far.start()
    up_near.start()
    gate_far.wait_recv()
    gate_on.start()

    wait_bytes(res_all.at[core], n_half - 1, recv_sem.at[4])
    res_on = pltpu.make_async_remote_copy(
        src_ref=res_all.at[core],
        dst_ref=res_all.at[core],
        send_sem=bulk_send.at[7],
        recv_sem=bulk_recv.at[7],
        device_id=(i, near),
        device_id_type=MESH,
    )
    res_on.start()

    wait_bytes(rw_all, n_ep - 1, recv_sem.at[1])
    wide = (n_ep, seq, rw_all.shape[-1])
    diag = lax.broadcasted_iota(jnp.int32, wide, 1) == lax.broadcasted_iota(jnp.int32, wide, 2)
    weight = jnp.where(diag, jnp.broadcast_to(rw_all[...], wide), 0.0)
    weight = jnp.sum(weight.reshape(n_ep * seq, -1), axis=-1, keepdims=True)
    wait_bytes(dm_all, n_tp - 1, recv_sem.at[2])

    res_on.wait_recv()
    rows = res_all[...].reshape(2, n_ep, half, seq, quarter)
    parts = [
        rows[k % 2, :, k // 2].reshape(n_ep * seq, quarter).astype(F32) for k in range(n_tp)
    ]
    square = sum(jnp.sum(p * p, axis=-1, keepdims=True) for p in parts)
    scale = lax.rsqrt(square / (n_tp * quarter) + EPS)
    logit = jnp.zeros_like(scale)
    for k in range(n_tp):
        cols = slice(k * quarter, (k + 1) * quarter)
        part = (parts[k] * scale * gain_ffn[:, cols]).astype(BF16)
        xs[:, cols] = part
        logit += jnp.sum(part.astype(F32) * dm_all[k][0:1, :], axis=-1, keepdims=True)
    mix_gate = jax.nn.sigmoid(logit)

    got_eg.wait()
    got_eu.wait()
    g = dot_t(xs[...], eg[...])
    u = dot_t(xs[...], eu[...])
    hidden = (g * jax.nn.sigmoid(g) * u).astype(BF16)
    up_far.wait_recv()
    up_on.start()
    got_ed.wait()
    def expert_part(tp_index):
        cols = pl.ds(pl.multiple_of(tp_index * quarter, quarter), quarter)
        return dot(hidden, ed[:, cols]) * weight

    for k in range(half):
        give[k] = expert_part(2 * k + 1 - core).astype(BF16).reshape(n_ep, seq, quarter)
    give_on = pltpu.make_async_remote_copy(
        src_ref=give,
        dst_ref=take,
        send_sem=bulk_send.at[6],
        recv_sem=bulk_recv.at[6],
        device_id=(i, near),
        device_id_type=MESH,
    )
    give_on.start()
    kept = [expert_part(2 * k + core) for k in range(half)]

    got_dg.wait()
    gate_near.wait_recv()
    gate_on.wait_recv()
    g = dot(xs[...], dg[...].reshape(n_tp * quarter, -1))
    got_du.wait()
    up_near.wait_recv()
    up_on.wait_recv()
    u = dot(xs[...], du[...].reshape(n_tp * quarter, -1))
    hidden = (g * jax.nn.sigmoid(g) * u).astype(BF16)
    got_dd.wait()
    dense = dot(hidden, dd[...]) * mix_gate
    give_on.wait_recv()
    for k in range(half):
        total = kept[k] + jnp.where(j // 2 == k, dense, 0.0)
        total += take[k].reshape(n_ep * seq, quarter).astype(F32)
        c_out[k] = total.astype(BF16).reshape(n_ep, seq, quarter)
    c_in[mine] = c_out[j // 2, i]

    def send_back(step, carry):
        peer = lax.rem(mine + step, n_half)
        pi, px = peer // half, lax.rem(peer, half)
        pltpu.make_async_remote_copy(
            src_ref=c_out.at[px, pi],
            dst_ref=c_in.at[mine],
            send_sem=send_sem.at[5],
            recv_sem=recv_sem.at[5],
            device_id=(pi, 2 * px + core),
            device_id_type=MESH,
        ).start()
        return carry

    lax.fori_loop(1, n_half, send_back, 0)

    wait_bytes(tok_all, n_tp - 1, send_sem.at[0])
    wait_bytes(rw_all, n_ep - 1, send_sem.at[1])
    wait_bytes(dm_all, n_tp - 1, send_sem.at[2])
    wait_bytes(mix_all, n_tp - 1, send_sem.at[3])
    wait_bytes(res_all.at[core], n_half - 1, send_sem.at[4])
    for copy in (gate_far, gate_near, gate_on, up_far, up_near, up_on, give_on, res_on):
        copy.wait_send()

    wait_bytes(c_in, n_half - 1, recv_sem.at[5])

    def add(k, total):
        return total + c_in[k].astype(F32)

    total = lax.fori_loop(0, n_half, add, res_own[...].astype(F32), unroll=8)
    out[...] = total.astype(BF16)
    wait_bytes(c_in, n_half - 1, send_sem.at[5])


def local(
    n_ep,
    n_tp,
    tokens,
    gain_mix,
    w_query,
    w_key,
    w_value,
    w_outgate,
    w_input_gate,
    w_forget_gate,
    w_mix_out,
    cell_state,
    norm_state,
    max_state,
    gain_ffn,
    route_ids,
    route_logits,
    expert_gate,
    expert_up,
    expert_down,
    dense_gate,
    dense_up,
    dense_down,
    dense_mix,
):
    seq, quarter = tokens.shape
    features, head = w_query.shape
    n_all = n_ep * n_tp
    ff = expert_gate.shape[2]
    dff = dense_gate.shape[1]
    vmem = pl.BlockSpec(memory_space=pltpu.VMEM)
    any_space = pl.BlockSpec(memory_space=pl.ANY)
    small = (
        tokens,
        gain_mix.reshape(1, -1),
        w_input_gate.reshape(1, -1),
        w_forget_gate.reshape(1, -1),
        norm_state.reshape(seq, head),
        max_state.T,
        gain_ffn.reshape(1, -1),
        route_ids.T,
        route_logits.T,
        dense_mix.reshape(-1, 128),
    )
    large = (
        w_query,
        w_key,
        w_value,
        w_outgate,
        w_mix_out,
        cell_state.reshape(seq, head, head),
        jnp.swapaxes(expert_gate, 1, 2),
        jnp.swapaxes(expert_up, 1, 2),
        expert_down,
        dense_gate,
        dense_up,
        dense_down,
    )
    return pl.pallas_call(
        functools.partial(kernel, n_ep, n_tp),
        out_shape=jax.ShapeDtypeStruct((seq, quarter), BF16),
        in_specs=[vmem] * len(small) + [any_space] * len(large),
        out_specs=vmem,
        scratch_shapes=[
            pltpu.VMEM((features, 4 * head), BF16),
            pltpu.VMEM(w_mix_out.shape, BF16),
            pltpu.VMEM((seq, head, head), F32),
            pltpu.VMEM((ff, features), BF16),
            pltpu.VMEM((ff, features), BF16),
            pltpu.VMEM((ff, features), BF16),
            pltpu.VMEM((n_tp, quarter, dff), BF16),
            pltpu.VMEM((n_tp, quarter, dff), BF16),
            pltpu.VMEM(dense_down.shape, BF16),
            pltpu.VMEM((n_tp, seq, quarter), BF16),
            pltpu.VMEM((n_tp, seq, head), BF16),
            pltpu.VMEM((seq, head), BF16),
            pltpu.VMEM((8, quarter), F32),
            pltpu.VMEM((n_tp, 8, quarter), F32),
            pltpu.VMEM((n_ep, 1, 128), F32),
            pltpu.VMEM((n_ep, 1, 128), F32),
            pltpu.VMEM((seq, quarter), BF16),
            pltpu.VMEM((2, n_all // 2, seq, quarter), BF16),
            pltpu.VMEM((n_ep * seq, features), BF16),
            pltpu.VMEM((seq, head), F32),
            pltpu.VMEM((n_tp // 2, n_ep, seq, quarter), BF16),
            pltpu.VMEM((n_tp // 2, n_ep, seq, quarter), BF16),
            pltpu.VMEM((n_tp // 2, n_ep, seq, quarter), BF16),
            pltpu.VMEM((n_all // 2, seq, quarter), BF16),
            pltpu.SemaphoreType.DMA((12,)),
            pltpu.SemaphoreType.DMA((6,)),
            pltpu.SemaphoreType.DMA((6,)),
            pltpu.SemaphoreType.DMA((8,)),
            pltpu.SemaphoreType.DMA((8,)),
            pltpu.SemaphoreType.REGULAR((n_ep.bit_length() - 1,)),
        ],
        compiler_params=pltpu.CompilerParams(
            collective_id=0, has_side_effects=True, vmem_limit_bytes=60 * 1024 * 1024
        ),
    )(*small, *large)


def solution(mesh):
    return jax.shard_map(
        functools.partial(local, mesh.shape["ep"], mesh.shape["tp"]),
        mesh=mesh,
        in_specs=(
            P("ep", "tp"),
            P(),
            P(None, "tp"),
            P(None, "tp"),
            P(None, "tp"),
            P(None, "tp"),
            P(None, "tp"),
            P(None, "tp"),
            P(None, "tp"),
            P("ep", "tp", None, None),
            P("ep", "tp", None),
            P("ep", "tp"),
            P(),
            P("ep", None),
            P("ep", None),
            P("ep", None, "tp"),
            P("ep", None, "tp"),
            P("ep", "tp", None),
            P("tp", "ep"),
            P("tp", "ep"),
            P("ep", "tp"),
            P("tp"),
        ),
        out_specs=P("ep", "tp"),
        check_vma=False,
    )
```

```python
import functools

import jax
import jax.numpy as jnp
from jax import lax
from jax.experimental import pallas as pl
from jax.experimental.pallas import tpu as pltpu
from jax.sharding import PartitionSpec as P

F32 = jnp.float32
BF16 = jnp.bfloat16
MESH = pl.DeviceIdType.MESH
EPS = 1e-06


def dot(a, b):
    return jnp.dot(a, b, preferred_element_type=F32)


def dot_t(a, b):
    return lax.dot_general(a, b, (((1,), (1,)), ((), ())), preferred_element_type=F32)


def column(row):
    n = row.shape[1]
    square = (n, n)
    eye = lax.broadcasted_iota(jnp.int32, square, 0) == lax.broadcasted_iota(jnp.int32, square, 1)
    return jnp.sum(jnp.where(eye, jnp.broadcast_to(row, square), 0.0), axis=1, keepdims=True)


def kernel(
    n_ep,
    n_tp,
    tokens,
    gain_mix,
    w_ig,
    w_fg,
    norm_state,
    max_state,
    gain_ffn,
    ids,
    logits,
    dense_mix,
    w_q,
    w_k,
    w_v,
    w_o,
    w_mix,
    cell,
    e_gate,
    e_up,
    e_down,
    d_gate,
    d_up,
    d_down,
    out,
    wp,
    wm,
    cs,
    eg,
    eu,
    ed,
    dg,
    du,
    dd,
    tok_all,
    mix_all,
    mix_own,
    dm_own,
    dm_all,
    rw_own,
    rw_all,
    res_own,
    res_all,
    xs,
    read,
    give,
    take,
    c_out,
    c_in,
    local_sem,
    send_sem,
    recv_sem,
    bulk_send,
    bulk_recv,
    word_sem,
):
    i = lax.axis_index("ep")
    j = lax.axis_index("tp")
    seq, quarter = tokens.shape
    head = cs.shape[-1]

    local = []

    def fetch(src, dst):
        copy = pltpu.make_async_copy(src, dst, local_sem.at[len(local)])
        copy.start()
        local.append(copy)
        return copy

    barrier = pltpu.get_barrier_semaphore()

    flips = [i + b - 2 * b * lax.rem(i // b, 2) for b in (1 << k for k in range(n_ep.bit_length() - 1))]
    hello = [(i, lax.rem(j + step, n_tp)) for step in range(1, n_tp)] + [(f, j) for f in flips]
    for peer in hello:
        pl.semaphore_signal(barrier, inc=1, device_id=peer, device_id_type=MESH)

    def tell(k):
        pl.semaphore_signal(word_sem.at[k], inc=1, device_id=(flips[k], j), device_id_type=MESH)

    def hear(k):
        pl.semaphore_wait(word_sem.at[k], 1)

    got_proj = [
        fetch(w, wp.at[:, pl.ds(k * head, head)]) for k, w in enumerate((w_q, w_k, w_v, w_o))
    ]
    got_cell = fetch(cell, cs)
    got_mix = fetch(w_mix, wm)
    got_eg = fetch(e_gate.at[0], eg)
    got_eu = fetch(e_up.at[0], eu)
    got_ed = fetch(e_down.at[0], ed)
    got_dg = fetch(d_gate, dg.at[j])
    got_du = fetch(d_up, du.at[j])
    got_dd = fetch(d_down, dd)

    l0, l1 = logits[0:1, :], logits[1:2, :]
    s0, s1 = jax.nn.sigmoid(l0 - l1), jax.nn.sigmoid(l1 - l0)

    def put_rw(e, carry):
        rw_own[e, :, 0:seq] = jnp.where(ids[0:1, :] == e, s0, 0.0) + jnp.where(
            ids[1:2, :] == e, s1, 0.0
        )
        return carry

    rw_own[...] = jnp.zeros_like(rw_own)
    lax.fori_loop(0, n_ep, put_rw, 0, unroll=8)
    rw_all[i] = rw_own[i]
    mix_row = dense_mix[...].astype(F32)
    mix_row = jnp.concatenate([mix_row[k : k + 1] for k in range(mix_row.shape[0])], axis=1)
    dm_own[...] = jnp.broadcast_to(mix_row, dm_own.shape)
    dm_all[j] = dm_own[...]
    tok_all[j] = tokens[...]

    pl.semaphore_wait(barrier, len(hello))
    tell(0)

    def to_tp(src, dst, phase):
        for step in range(1, n_tp):
            pltpu.make_async_remote_copy(
                src_ref=src,
                dst_ref=dst.at[j],
                send_sem=send_sem.at[phase],
                recv_sem=recv_sem.at[phase],
                device_id=(i, lax.rem(j + step, n_tp)),
                device_id_type=MESH,
            ).start()

    def wait_bytes(buf, count, sem):
        view = buf.at[pl.ds(0, count)]
        pltpu.make_async_copy(view, view, sem).wait()

    to_tp(tokens, tok_all, 0)

    near = j + 1 - 2 * lax.rem(j, 2)
    far = lax.rem(j + 2, n_tp)

    def bulk(src, buf, slot, peer, k):
        return pltpu.make_async_remote_copy(
            src_ref=src,
            dst_ref=buf.at[slot],
            send_sem=bulk_send.at[k],
            recv_sem=bulk_recv.at[k],
            device_id=(i, peer),
            device_id_type=MESH,
        )

    gate_far = bulk(d_gate, dg, j, far, 0)
    gate_near = bulk(d_gate, dg, j, near, 1)
    gate_on = bulk(dg.at[far], dg, far, near, 2)
    up_far = bulk(d_up, du, j, far, 3)
    up_near = bulk(d_up, du, j, near, 4)
    up_on = bulk(du.at[far], du, far, near, 5)
    gate_far.start()
    gate_near.start()

    def send_rw(step, carry):
        e = lax.rem(i + step, n_ep)
        pltpu.make_async_remote_copy(
            src_ref=rw_own.at[e],
            dst_ref=rw_all.at[i],
            send_sem=send_sem.at[1],
            recv_sem=recv_sem.at[1],
            device_id=(e, j),
            device_id_type=MESH,
        ).start()
        return carry

    to_tp(dm_own, dm_all, 2)

    wait_bytes(tok_all, n_tp - 1, recv_sem.at[0])
    hear(0)
    tell(1)
    full = jnp.concatenate([tok_all[k] for k in range(n_tp)], axis=1).astype(F32)
    scale = lax.rsqrt(jnp.mean(full * full, axis=-1, keepdims=True) + EPS)
    normed = (full * scale * gain_mix[...]).astype(BF16)
    normed_f = normed.astype(F32)
    ig = jnp.sum(normed_f * w_ig[...].astype(F32), axis=-1, keepdims=True)
    fg = jnp.sum(normed_f * w_fg[...].astype(F32), axis=-1, keepdims=True)
    for copy in got_proj:
        copy.wait()
    proj = dot(normed, wp[...])
    query = proj[:, :head]
    key = proj[:, head : 2 * head] * head ** (-0.5)
    value = proj[:, 2 * head : 3 * head]
    out_gate = proj[:, 3 * head :]
    carried = jnp.minimum(fg, 0.0) - jnp.log1p(jnp.exp(-jnp.abs(fg))) + column(max_state[...])
    stab = jnp.maximum(carried, ig)
    w_old = jnp.exp(carried - stab)
    w_new = jnp.exp(ig - stab) * jnp.sum(query * key, axis=-1, keepdims=True)
    got_cell.wait()
    query_t = query.T
    for b in range(seq):
        read[b : b + 1, :] = jnp.sum(query_t[:, b : b + 1] * cs[b], axis=0, keepdims=True)
    numer = w_old * read[...] + w_new * value
    denom = w_old * jnp.sum(query * norm_state[...], axis=-1, keepdims=True) + w_new
    cell_out = numer / jnp.maximum(jnp.abs(denom), 1.0)
    mixed = (jax.nn.sigmoid(out_gate) * cell_out).astype(BF16)
    mix_own[...] = mixed
    mix_all[j] = mixed
    to_tp(mix_own, mix_all, 3)
    for k in range(1, len(flips) - 1):
        hear(k)
        tell(k + 1)
    got_mix.wait()
    wait_bytes(mix_all, n_tp - 1, recv_sem.at[3])
    heads = jnp.concatenate([mix_all[k] for k in range(n_tp)], axis=1)
    resid = (tokens[...].astype(F32) + dot(heads, wm[...])).astype(BF16)
    res_own[...] = resid
    core = lax.rem(j, 2)
    half = n_tp // 2
    n_half = n_ep * half
    mine = i * half + j // 2
    res_all[core, mine] = resid

    def send_res(step, carry):
        peer = lax.rem(mine + step, n_half)
        pltpu.make_async_remote_copy(
            src_ref=res_own,
            dst_ref=res_all.at[core, mine],
            send_sem=send_sem.at[4],
            recv_sem=recv_sem.at[4],
            device_id=(peer // half, 2 * lax.rem(peer, half) + core),
            device_id_type=MESH,
        ).start()
        return carry

    hear(len(flips) - 1)
    lax.fori_loop(1, n_half, send_res, 0)
    lax.fori_loop(1, n_ep, send_rw, 0)
    up_far.start()
    up_near.start()
    gate_far.wait_recv()
    gate_on.start()

    wait_bytes(res_all.at[core], n_half - 1, recv_sem.at[4])
    res_on = pltpu.make_async_remote_copy(
        src_ref=res_all.at[core],
        dst_ref=res_all.at[core],
        send_sem=bulk_send.at[7],
        recv_sem=bulk_recv.at[7],
        device_id=(i, near),
        device_id_type=MESH,
    )
    res_on.start()

    wait_bytes(rw_all, n_ep - 1, recv_sem.at[1])
    wide = (n_ep, seq, rw_all.shape[-1])
    diag = lax.broadcasted_iota(jnp.int32, wide, 1) == lax.broadcasted_iota(jnp.int32, wide, 2)
    weight = jnp.where(diag, jnp.broadcast_to(rw_all[...], wide), 0.0)
    weight = jnp.sum(weight.reshape(n_ep * seq, -1), axis=-1, keepdims=True)
    wait_bytes(dm_all, n_tp - 1, recv_sem.at[2])

    res_on.wait_recv()
    rows = res_all[...].reshape(2, n_ep, half, seq, quarter)
    parts = [
        rows[k % 2, :, k // 2].reshape(n_ep * seq, quarter).astype(F32) for k in range(n_tp)
    ]
    square = sum(jnp.sum(p * p, axis=-1, keepdims=True) for p in parts)
    scale = lax.rsqrt(square / (n_tp * quarter) + EPS)
    logit = jnp.zeros_like(scale)
    for k in range(n_tp):
        cols = slice(k * quarter, (k + 1) * quarter)
        part = (parts[k] * scale * gain_ffn[:, cols]).astype(BF16)
        xs[:, cols] = part
        logit += jnp.sum(part.astype(F32) * dm_all[k][0:1, :], axis=-1, keepdims=True)
    mix_gate = jax.nn.sigmoid(logit)

    got_eg.wait()
    got_eu.wait()
    g = dot_t(xs[...], eg[...])
    u = dot_t(xs[...], eu[...])
    hidden = (g * jax.nn.sigmoid(g) * u).astype(BF16)
    up_far.wait_recv()
    up_on.start()
    got_ed.wait()
    def expert_part(tp_index):
        cols = pl.ds(pl.multiple_of(tp_index * quarter, quarter), quarter)
        return dot(hidden, ed[:, cols]) * weight

    for k in range(half):
        give[k] = expert_part(2 * k + 1 - core).astype(BF16).reshape(n_ep, seq, quarter)
    give_on = pltpu.make_async_remote_copy(
        src_ref=give,
        dst_ref=take,
        send_sem=bulk_send.at[6],
        recv_sem=bulk_recv.at[6],
        device_id=(i, near),
        device_id_type=MESH,
    )
    give_on.start()
    kept = [expert_part(2 * k + core) for k in range(half)]

    got_dg.wait()
    gate_near.wait_recv()
    gate_on.wait_recv()
    g = dot(xs[...], dg[...].reshape(n_tp * quarter, -1))
    got_du.wait()
    up_near.wait_recv()
    up_on.wait_recv()
    u = dot(xs[...], du[...].reshape(n_tp * quarter, -1))
    hidden = (g * jax.nn.sigmoid(g) * u).astype(BF16)
    got_dd.wait()
    dense = dot(hidden, dd[...]) * mix_gate
    give_on.wait_recv()
    for k in range(half):
        total = kept[k] + jnp.where(j // 2 == k, dense, 0.0)
        total += take[k].reshape(n_ep * seq, quarter).astype(F32)
        c_out[k] = total.astype(BF16).reshape(n_ep, seq, quarter)
    c_in[mine] = c_out[j // 2, i]

    def send_back(step, carry):
        peer = lax.rem(mine + step, n_half)
        pi, px = peer // half, lax.rem(peer, half)
        pltpu.make_async_remote_copy(
            src_ref=c_out.at[px, pi],
            dst_ref=c_in.at[mine],
            send_sem=send_sem.at[5],
            recv_sem=recv_sem.at[5],
            device_id=(pi, 2 * px + core),
            device_id_type=MESH,
        ).start()
        return carry

    lax.fori_loop(1, n_half, send_back, 0)

    wait_bytes(tok_all, n_tp - 1, send_sem.at[0])
    wait_bytes(rw_all, n_ep - 1, send_sem.at[1])
    wait_bytes(dm_all, n_tp - 1, send_sem.at[2])
    wait_bytes(mix_all, n_tp - 1, send_sem.at[3])
    wait_bytes(res_all.at[core], n_half - 1, send_sem.at[4])
    for copy in (gate_far, gate_near, gate_on, up_far, up_near, up_on, give_on, res_on):
        copy.wait_send()

    wait_bytes(c_in, n_half - 1, recv_sem.at[5])

    def add(k, total):
        return total + c_in[k].astype(F32)

    total = lax.fori_loop(0, n_half, add, res_own[...].astype(F32), unroll=8)
    out[...] = total.astype(BF16)
    wait_bytes(c_in, n_half - 1, send_sem.at[5])


def local(
    n_ep,
    n_tp,
    tokens,
    gain_mix,
    w_query,
    w_key,
    w_value,
    w_outgate,
    w_input_gate,
    w_forget_gate,
    w_mix_out,
    cell_state,
    norm_state,
    max_state,
    gain_ffn,
    route_ids,
    route_logits,
    expert_gate,
    expert_up,
    expert_down,
    dense_gate,
    dense_up,
    dense_down,
    dense_mix,
):
    seq, quarter = tokens.shape
    features, head = w_query.shape
    n_all = n_ep * n_tp
    ff = expert_gate.shape[2]
    dff = dense_gate.shape[1]
    vmem = pl.BlockSpec(memory_space=pltpu.VMEM)
    any_space = pl.BlockSpec(memory_space=pl.ANY)
    small = (
        tokens,
        gain_mix.reshape(1, -1),
        w_input_gate.reshape(1, -1),
        w_forget_gate.reshape(1, -1),
        norm_state.reshape(seq, head),
        max_state.T,
        gain_ffn.reshape(1, -1),
        route_ids.T,
        route_logits.T,
        dense_mix.reshape(-1, 128),
    )
    large = (
        w_query,
        w_key,
        w_value,
        w_outgate,
        w_mix_out,
        cell_state.reshape(seq, head, head),
        jnp.swapaxes(expert_gate, 1, 2),
        jnp.swapaxes(expert_up, 1, 2),
        expert_down,
        dense_gate,
        dense_up,
        dense_down,
    )
    return pl.pallas_call(
        functools.partial(kernel, n_ep, n_tp),
        out_shape=jax.ShapeDtypeStruct((seq, quarter), BF16),
        in_specs=[vmem] * len(small) + [any_space] * len(large),
        out_specs=vmem,
        scratch_shapes=[
            pltpu.VMEM((features, 4 * head), BF16),
            pltpu.VMEM(w_mix_out.shape, BF16),
            pltpu.VMEM((seq, head, head), F32),
            pltpu.VMEM((ff, features), BF16),
            pltpu.VMEM((ff, features), BF16),
            pltpu.VMEM((ff, features), BF16),
            pltpu.VMEM((n_tp, quarter, dff), BF16),
            pltpu.VMEM((n_tp, quarter, dff), BF16),
            pltpu.VMEM(dense_down.shape, BF16),
            pltpu.VMEM((n_tp, seq, quarter), BF16),
            pltpu.VMEM((n_tp, seq, head), BF16),
            pltpu.VMEM((seq, head), BF16),
            pltpu.VMEM((8, quarter), F32),
            pltpu.VMEM((n_tp, 8, quarter), F32),
            pltpu.VMEM((n_ep, 1, 128), F32),
            pltpu.VMEM((n_ep, 1, 128), F32),
            pltpu.VMEM((seq, quarter), BF16),
            pltpu.VMEM((2, n_all // 2, seq, quarter), BF16),
            pltpu.VMEM((n_ep * seq, features), BF16),
            pltpu.VMEM((seq, head), F32),
            pltpu.VMEM((n_tp // 2, n_ep, seq, quarter), BF16),
            pltpu.VMEM((n_tp // 2, n_ep, seq, quarter), BF16),
            pltpu.VMEM((n_tp // 2, n_ep, seq, quarter), BF16),
            pltpu.VMEM((n_all // 2, seq, quarter), BF16),
            pltpu.SemaphoreType.DMA((12,)),
            pltpu.SemaphoreType.DMA((6,)),
            pltpu.SemaphoreType.DMA((6,)),
            pltpu.SemaphoreType.DMA((8,)),
            pltpu.SemaphoreType.DMA((8,)),
            pltpu.SemaphoreType.REGULAR((n_ep.bit_length() - 1,)),
        ],
        compiler_params=pltpu.CompilerParams(
            collective_id=0, has_side_effects=True, vmem_limit_bytes=60 * 1024 * 1024
        ),
    )(*small, *large)


def solution(mesh):
    return jax.shard_map(
        functools.partial(local, mesh.shape["ep"], mesh.shape["tp"]),
        mesh=mesh,
        in_specs=(
            P("ep", "tp"),
            P(),
            P(None, "tp"),
            P(None, "tp"),
            P(None, "tp"),
            P(None, "tp"),
            P(None, "tp"),
            P(None, "tp"),
            P(None, "tp"),
            P("ep", "tp", None, None),
            P("ep", "tp", None),
            P("ep", "tp"),
            P(),
            P("ep", None),
            P("ep", None),
            P("ep", None, "tp"),
            P("ep", None, "tp"),
            P("ep", "tp", None),
            P("tp", "ep"),
            P("tp", "ep"),
            P("ep", "tp"),
            P("tp"),
        ),
        out_specs=P("ep", "tp"),
        check_vma=False,
    )
```
